32 devices in a mesh: dp: 4 (over y, x), kv: 4 (over z), tp: 2 (over core).
Axes of the slice: x: 2, y: 2, z: 4, core: 2. Of those that a mesh axis runs over, the one named last changes fastest.
Arguments:
- tokens: bfloat16 [16, 4096], P('dp', ('kv', 'tp')), parts along dimension 0, may hold values from -6 to 6
- mix_gain: float32 [4096], replicated, may hold values from 0.1 to 1.9
- w_query: bfloat16 [4096, 2048], P('kv', 'tp'), may hold values from -0.09375 to 0.09375
- w_key: bfloat16 [4096, 2048], P('kv', 'tp'), may hold values from -0.09375 to 0.09375
- w_value: bfloat16 [4096, 4096], P('kv', 'tp'), may hold values from -0.09375 to 0.09375
- w_igate: bfloat16 [4096, 16], replicated, may hold values from -0.09375 to 0.09375
- w_fgate: bfloat16 [4096, 16], replicated, may hold values from -0.09375 to 0.09375
- igate_bias: float32 [16], replicated, may hold values from -3 to 1
- fgate_bias: float32 [16], replicated, may hold values from -2 to 5
- memory: float32 [16, 16, 256, 128], P(('dp', 'kv'), 'tp'), parts along dimension 0, may hold values from -6 to 6
- normalizer: float32 [16, 16, 128], P(('dp', 'kv'), 'tp'), parts along dimension 0, may hold values from -6 to 6
- stabilizer: float32 [16, 16], P(('dp', 'kv'), 'tp'), parts along dimension 0, may hold values from -3 to 3
- w_output: bfloat16 [4096, 4096], P('tp', 'kv'), may hold values from -0.09375 to 0.09375
- mlp_gain: float32 [4096], replicated, may hold values from 0.1 to 1.9
- w_up: bfloat16 [4096, 16384], P(None, ('kv', 'tp')), may hold values from -0.09375 to 0.09375
- w_down: bfloat16 [16384, 4096], P(('kv', 'tp')), may hold values from -0.0625 to 0.0625
Outputs:
- new_tokens: bfloat16 [16, 4096], P('dp', ('kv', 'tp')), parts along dimension 0
- new_memory: float32 [16, 16, 256, 128], P(('dp', 'kv'), 'tp'), parts along dimension 0
- new_normalizer: float32 [16, 16, 128], P(('dp', 'kv'), 'tp'), parts along dimension 0
- new_stabilizer: float32 [16, 16], P(('dp', 'kv'), 'tp'), parts along dimension 0
The draws below stay inside these ranges and needn't reach their ends.
There are 4 independent parts, one for each index of `dp`. The reference program is written for one: setup_inputs(seed, part) draws one part's arguments, and reference() takes and returns one part's arrays. A program takes and returns all parts, laid end to end along the dimension named above; an argument that names none is the same for every part. Nothing has to cross between parts.
All inputs are finite; a program needn't handle non-finite values.
Results may differ from the reference program's by a relative error of at most 0.019.
Values may be sent and summed in bfloat16 or wider, within the bound.
A program may use at most 128 MiB of HBM per device.

```python
import jax
import jax.numpy as jnp
from jax import lax

D = 4096
NH = 16
DV = 256
DQK = 128
FF = 16384
BATCH = 4
N_TP = 2


def with_spikes(array, key, source, target, shards_of, factor):
    def block_of(axis_at):
        return (jnp.arange(array.shape[axis_at]) // (array.shape[axis_at] // shards_of)).reshape((-1,) + (1,) * (array.ndim - 1 - axis_at))

    near = jax.random.permutation(key, shards_of)[block_of(target)]
    far = (block_of(target) + shards_of // 2) % shards_of
    return jnp.where((block_of(source) == near) | (block_of(source) == far), factor * array, array)


def levels(stream_key, shape, split, least, high):
    level, own = 1.0, jax.random.fold_in(stream_key, 6)
    for position, parts in split:
        heights = jnp.exp(jax.random.uniform(jax.random.fold_in(own, position), (parts,), jnp.float32, least / len(split), high / len(split)))
        level = level * jnp.repeat(heights, shape[position] // parts).reshape([-1 if axis == position else 1 for axis in range(len(shape))])
    return level


def bell_draw(stream_key, dims, width, most, cuts=(), dtype=jnp.bfloat16):
    values = jax.random.normal(stream_key, dims, jnp.float32) * width
    if len(cuts) > 0:
        values = levels(stream_key, dims, cuts, -0.22, 0.18) * values
    return jnp.clip(values, min=-most, max=most).astype(dtype)


def gaussian_with(key, shape, spread, reach, cuts, heavy, dtype=jnp.bfloat16):
    drawn = spread * jax.random.normal(key, shape, jnp.float32)
    if cuts:
        drawn = drawn * levels(key, shape, cuts, -0.22, 0.18)
    return jnp.clip(with_spikes(drawn, jax.random.fold_in(key, 3), *heavy), -reach, reach).astype(dtype)


def setup_inputs(seed: int = 0, part: int = 0) -> dict:
    key_of = jax.random.split(jax.random.key(seed), 17)
    part_splits = jax.random.split(jax.random.fold_in(key_of[16], part), 17)
    tokens = gaussian_with(part_splits[0], (BATCH, D), 1.0, 6.0, ((1, 8),), (1, 0, 4, 2.0))
    mix_gain = jnp.clip(1.0 + 0.18 * jax.random.normal(key_of[1], (D,), jnp.float32), 0.1, 1.9)
    w_query = bell_draw(key_of[2], (D, NH * DQK), D ** -0.5, 0.09375, ((0, 4), (1, 2)))
    w_key = bell_draw(key_of[3], (D, NH * DQK), D ** -0.5, 0.09375, ((0, 4), (1, 2)))
    w_value = bell_draw(key_of[4], (D, NH * DV), D ** -0.5, 0.09375, ((0, 4), (1, 2)))
    w_igate = bell_draw(key_of[5], (D, NH), D ** -0.5, 0.09375)
    w_fgate = bell_draw(key_of[6], (D, NH), D ** -0.5, 0.09375)
    igate_bias = jnp.clip(jax.random.uniform(key_of[7], (NH,), jnp.float32, -3.0, 1.0), -3.0, 1.0)
    fgate_bias = jnp.clip(jax.random.uniform(key_of[8], (NH,), jnp.float32, -2.0, 5.0), -2.0, 5.0)
    memory = bell_draw(part_splits[9], (BATCH, NH, DV, DQK), 1.0, 6.0, ((0, 4), (1, 2)), jnp.float32)
    normalizer = bell_draw(part_splits[10], (BATCH, NH, DQK), 1.0, 6.0, ((0, 4), (1, 2)), jnp.float32)
    stabilizer = jnp.clip(jax.random.uniform(part_splits[11], (BATCH, NH), jnp.float32, -3.0, 3.0) * levels(part_splits[11], (BATCH, NH), ((0, 4), (1, 2)), -0.4, 0.0), -3.0, 3.0)
    w_output = bell_draw(key_of[12], (NH * DV, D), (NH * DV) ** -0.5, 0.09375, ((0, 2), (1, 4)))
    mlp_gain = jnp.clip(1.0 + 0.18 * jax.random.normal(key_of[13], (D,), jnp.float32), 0.1, 1.9)
    w_up = bell_draw(key_of[14], (D, FF), D ** -0.5, 0.09375, ((1, 8),))
    w_down = gaussian_with(key_of[15], (FF, D), FF ** -0.5, 0.0625, ((0, 8),), (0, 1, 8, 2.0))
    return {"tokens": tokens, "mix_gain": mix_gain, "w_query": w_query, "w_key": w_key, "w_value": w_value, "w_igate": w_igate, "w_fgate": w_fgate, "igate_bias": igate_bias, "fgate_bias": fgate_bias, "memory": memory, "normalizer": normalizer, "stabilizer": stabilizer, "w_output": w_output, "mlp_gain": mlp_gain, "w_up": w_up, "w_down": w_down}


norm_eps = 1e-06

def rms_normed(rows, gain):
    wide_rows = rows.astype(jnp.float32)
    scale = lax.rsqrt(lax.optimization_barrier(jnp.mean(wide_rows * wide_rows, axis=-1, keepdims=True)) + norm_eps)
    return (wide_rows * scale * gain).astype(jnp.bfloat16)

def reference(tokens, mix_gain, w_query, w_key, w_value, w_igate, w_fgate, igate_bias, fgate_bias, memory, normalizer, stabilizer, w_output, mlp_gain, w_up, w_down):
    batch_rows = tokens.shape[0]
    normed = rms_normed(tokens, mix_gain)
    queries = (jnp.dot(normed, w_query, preferred_element_type=jnp.float32) * DQK ** (-0.5)).reshape(batch_rows, NH, DQK)
    key_rows = jnp.dot(normed, w_key, preferred_element_type=jnp.float32).reshape(batch_rows, NH, DQK)
    values = jnp.dot(normed, w_value, preferred_element_type=jnp.float32).reshape(batch_rows, NH, DV)
    input_gate = jnp.dot(normed, w_igate, preferred_element_type=jnp.float32) + igate_bias
    log_forget = jax.nn.log_sigmoid(jnp.dot(normed, w_fgate, preferred_element_type=jnp.float32) + fgate_bias)
    carried = log_forget + stabilizer
    new_stabilizer = jnp.maximum(carried, input_gate)
    keep_weight = jnp.exp(carried - new_stabilizer)
    fresh_weight = jnp.exp(input_gate - new_stabilizer)
    recall = jnp.einsum('bhvd,bhd->bhv', memory, queries, precision=lax.Precision.HIGHEST)
    match_score = lax.optimization_barrier(jnp.sum(queries * key_rows, axis=-1))
    numerator = keep_weight[..., None] * recall + (fresh_weight * match_score)[..., None] * values
    denominator = keep_weight * lax.optimization_barrier(jnp.sum(normalizer * queries, axis=-1)) + fresh_weight * match_score
    floor_value = jnp.maximum(jnp.abs(denominator), jnp.exp(-new_stabilizer))
    cell_out = (numerator / floor_value[..., None]).astype(jnp.bfloat16).reshape(batch_rows, NH * DV)
    new_memory = keep_weight[..., None, None] * memory + fresh_weight[..., None, None] * values[..., :, None] * key_rows[..., None, :]
    new_normalizer = keep_weight[..., None] * normalizer + fresh_weight[..., None] * key_rows
    half_width = NH * DV // N_TP
    summed = tokens.astype(jnp.float32)
    for half_index in range(N_TP):
        half_out = jnp.dot(cell_out[:, half_index * half_width:(half_index + 1) * half_width], w_output[half_index * half_width:(half_index + 1) * half_width], preferred_element_type=jnp.float32).astype(jnp.bfloat16)
        half_out = lax.optimization_barrier(half_out)
        summed = summed + half_out.astype(jnp.float32)
    middle = summed.astype(jnp.bfloat16)
    mixer_in = rms_normed(middle, mlp_gain)
    up_rows = jnp.dot(mixer_in, w_up, preferred_element_type=jnp.float32)
    activation = jnp.square(jax.nn.relu(up_rows)).astype(jnp.bfloat16)
    down_rows = jnp.dot(activation, w_down, preferred_element_type=jnp.float32)
    new_tokens = (middle.astype(jnp.float32) + down_rows).astype(jnp.bfloat16)
    return (new_tokens, new_memory, new_normalizer, new_stabilizer)
```

```python
import functools

import jax
import jax.numpy as jnp
from jax import lax
from jax.experimental import pallas as pl
from jax.experimental.pallas import tpu as pltpu
from jax.sharding import PartitionSpec as P

MESH = pl.DeviceIdType.MESH
F32 = jnp.float32
BF16 = jnp.bfloat16
LANES = 128


norm_eps = 1e-06


def rms_normed(rows, gain):
    wide_rows = rows.astype(jnp.float32)
    scale = lax.rsqrt(jnp.mean(wide_rows * wide_rows, axis=-1, keepdims=True) + norm_eps)
    return (wide_rows * scale * gain).astype(jnp.bfloat16)


def on_device(
    tokens,
    mix_gain,
    w_query,
    w_key,
    w_value,
    w_igate,
    w_fgate,
    igate_bias,
    fgate_bias,
    memory,
    normalizer,
    stabilizer,
    w_output,
    mlp_gain,
    w_up,
    w_down,
):
    DV, DQK = memory.shape[2:]
    kv_count = lax.axis_size("kv")
    tp_count = lax.axis_size("tp")
    kv_index = lax.axis_index("kv")
    tp_index = lax.axis_index("tp")
    own_rows = memory.shape[0]
    head_count = memory.shape[1]
    whole_rows = lax.all_gather(tokens, ("kv", "tp"), axis=1, tiled=True)
    batch_rows = whole_rows.shape[0]
    wide_rows = whole_rows.astype(jnp.float32)
    normed = rms_normed(whole_rows, mix_gain)
    row_span = w_query.shape[0]
    own_cols = lax.dynamic_slice_in_dim(normed, kv_index * row_span, row_span, 1)
    joined = lax.psum_scatter(
        jnp.concatenate(
            [
                jnp.dot(own_cols, w_query, preferred_element_type=jnp.float32),
                jnp.dot(own_cols, w_key, preferred_element_type=jnp.float32),
                jnp.dot(own_cols, w_value, preferred_element_type=jnp.float32),
            ],
            axis=1,
        ),
        "kv",
        scatter_dimension=0,
        tiled=True,
    )
    query_cols = w_query.shape[1]
    queries = joined[:, :query_cols].reshape(own_rows, head_count, DQK) * DQK ** (-0.5)
    key_rows = joined[:, query_cols : 2 * query_cols].reshape(own_rows, head_count, DQK)
    values = joined[:, 2 * query_cols :].reshape(own_rows, head_count, DV)
    own_normed = lax.dynamic_slice_in_dim(normed, kv_index * own_rows, own_rows, 0)
    igate_cols = lax.dynamic_slice_in_dim(w_igate, tp_index * head_count, head_count, 1)
    fgate_cols = lax.dynamic_slice_in_dim(w_fgate, tp_index * head_count, head_count, 1)
    ibias_own = lax.dynamic_slice_in_dim(igate_bias, tp_index * head_count, head_count, 0)
    fbias_own = lax.dynamic_slice_in_dim(fgate_bias, tp_index * head_count, head_count, 0)
    input_gate = jnp.dot(own_normed, igate_cols, preferred_element_type=jnp.float32) + ibias_own
    log_forget = jax.nn.log_sigmoid(
        jnp.dot(own_normed, fgate_cols, preferred_element_type=jnp.float32) + fbias_own
    )
    carried = log_forget + stabilizer
    new_stabilizer = jnp.maximum(carried, input_gate)
    keep_weight = jnp.exp(carried - new_stabilizer)
    fresh_weight = jnp.exp(input_gate - new_stabilizer)
    recall = jnp.einsum("bhvd,bhd->bhv", memory, queries, precision=lax.Precision.HIGHEST)
    match_score = jnp.sum(queries * key_rows, axis=-1)
    numerator = keep_weight[..., None] * recall + (fresh_weight * match_score)[..., None] * values
    denominator = keep_weight * jnp.sum(normalizer * queries, axis=-1) + fresh_weight * match_score
    floor_value = jnp.maximum(jnp.abs(denominator), jnp.exp(-new_stabilizer))
    cell_out = (
        (numerator / floor_value[..., None]).astype(jnp.bfloat16).reshape(own_rows, head_count * DV)
    )
    new_memory = (
        keep_weight[..., None, None] * memory
        + fresh_weight[..., None, None] * values[..., :, None] * key_rows[..., None, :]
    )
    new_normalizer = keep_weight[..., None] * normalizer + fresh_weight[..., None] * key_rows
    partial_value = jnp.dot(
        lax.all_gather(cell_out, "kv", axis=0, tiled=True),
        w_output,
        preferred_element_type=jnp.float32,
    )
    block_cols = partial_value.shape[1]
    pieces = lax.all_gather(
        partial_value.astype(jnp.bfloat16)[:, None, :], ("kv", "tp"), axis=1, tiled=True
    )
    summed = jnp.sum(
        pieces.astype(jnp.float32).reshape(batch_rows, kv_count, tp_count, block_cols), axis=2
    )
    middle = (wide_rows + summed.reshape(batch_rows, kv_count * block_cols)).astype(jnp.bfloat16)
    mixer_in = rms_normed(middle, mlp_gain)
    up_rows = jnp.dot(mixer_in, w_up, preferred_element_type=jnp.float32)
    activation = jnp.square(jax.nn.relu(up_rows)).astype(jnp.bfloat16)
    thin_cols = tokens.shape[1]
    down_cols = lax.psum_scatter(
        lax.dot_general(
            w_down, activation, (((0,), (1,)), ((), ())), preferred_element_type=jnp.float32
        ),
        ("kv", "tp"),
        scatter_dimension=0,
        tiled=True,
    )
    middle_own = lax.dynamic_slice_in_dim(
        middle, (kv_index * tp_count + tp_index) * thin_cols, thin_cols, 1
    )
    new_tokens = (middle_own.astype(jnp.float32) + down_cols.T).astype(jnp.bfloat16)
    return (new_tokens, new_memory, new_normalizer, new_stabilizer)


def landed(ref, sem):
    pltpu.make_async_copy(ref, ref, sem).wait()


def fused_cell(
    n_kv,
    n_tp,
    tok_h, mixg_h, wq_h, wk_h, wv_h, wig_h, wfg_h, ib_h, fb_h,
    mem_h, nrm_h, stb_h, wo_h, mlpg_h, wup_h, wdn_h,
    otok, newmem, onrm, ostb,
    tok, tokall, gains, wq, wk, wv, wg, bias,
    mem, membf, nrm, stb, wo, wup, wdn,
    own_part, part, snd, rcv, gsnd, grcv, vrow, cell_own, cell_all, y_own, y_all, mid, stage, land,
    load_sem, sent_sem, tok_r, rs_r, cell_r, y_r, dn_r,
):
    dp = lax.axis_index("dp")
    kv = lax.axis_index("kv")
    tp = lax.axis_index("tp")
    n_all = n_kv * n_tp
    g = kv * n_tp + tp
    batch, thin = tok.shape
    span = wq.shape[0]
    heads, dv, dqk = mem.shape
    width = n_all * thin
    halves = dv // LANES
    gate_count = wg.shape[0] // 2
    block = heads * LANES
    hidden = wup.shape[1]
    TOK_S, RS_S, GATE_S, CELL_S, Y_S, DN_S = range(6)

    def peer_of(offset):
        other = (g + offset) % n_all
        return dp, other // n_tp, other % n_tp

    own_span = pl.ds(pl.multiple_of(kv * span, span), span)

    def v_cols(p):
        return pl.ds(p * block, block)

    far_side = kv // 2
    near = kv + far_side * (3 - 2 * kv)

    def chip(i):
        if n_kv == 4:
            step = (i + near) % 3 if i < 3 else i
            return 3 * far_side + (1 - 2 * far_side) * step
        return (kv + i) % n_kv

    chips = [chip(i) for i in range(n_kv)]
    far_first = chips[:0:-1]

    def up_rows(j):
        return pl.ds(pl.multiple_of(j * span, span), span)

    TOK, GAINS, WQ, WK, WG, BIAS, NRM, STB, MEM, WO, WUP, WDN, WV = range(13)
    loads = [
        (tok_h, tok, TOK), (mixg_h, gains.at[0], GAINS), (mlpg_h, gains.at[1], GAINS), (wq_h, wq, WQ),
        (wk_h, wk, WK),
        (wig_h.at[:, own_span], wg.at[pl.ds(0, gate_count)], WG),
        (wfg_h.at[:, own_span], wg.at[pl.ds(gate_count, gate_count)], WG),
    ]
    loads += [(wv_h.at[:, v_cols(p)], wv.at[:, v_cols(p)], WV + p) for p in range(halves)]
    loads += [
        (ib_h, bias.at[0], BIAS), (fb_h, bias.at[1], BIAS), (nrm_h.at[0], nrm, NRM), (stb_h, stb, STB),
        (mem_h.at[0], mem, MEM), (wo_h, wo, WO),
    ]
    loads += [(wup_h.at[up_rows(j)], wup.at[up_rows(j)], WUP) for j in chips]
    loads += [(wdn_h, wdn, WDN)]
    load = [pltpu.make_async_copy(x, y, load_sem.at[n]) for x, y, n in loads]

    for c in load[:4]:
        c.start()
    barrier = pltpu.get_barrier_semaphore()
    for o in reversed(range(1, n_all)):
        pl.semaphore_signal(barrier, inc=1, device_id=peer_of(o), device_id_type=MESH)
    for c in load[4:]:
        c.start()

    gsnd[...] = jnp.zeros(gsnd.shape, F32)
    landed(tok, load_sem.at[TOK])
    pl.semaphore_wait(barrier, n_all - 1)

    def tok_copy(to, to_tp, n):
        return pltpu.make_async_remote_copy(
            src_ref=tok, dst_ref=tokall.at[g], send_sem=sent_sem.at[TOK_S], recv_sem=tok_r.at[n],
            device_id=(dp, to, to_tp), device_id_type=MESH)

    for t in range(1, n_tp):
        tok_copy(kv, (tp + t) % n_tp, 0).start()
    tokall[g] = tok[...]
    for to in far_first:
        for t in range(n_tp):
            tok_copy(to, (tp + t) % n_tp, 1).start()

    def chunk(t):
        cols = pl.ds(pl.multiple_of((kv * n_tp + t) * thin, thin), thin)
        raw = tokall[kv * n_tp + t].astype(F32)
        return (raw * gains[0, :, cols]).astype(BF16), jnp.sum(raw * raw, axis=1, keepdims=True)

    def product(x, t, w, cols):
        rows = pl.ds(pl.multiple_of(t * thin, thin), thin)
        return jnp.dot(x, w[rows, cols], preferred_element_type=F32)

    last = (((1,), (1,)), ((), ()))

    def gate_part(x, t):
        rows = pl.ds(pl.multiple_of(t * thin, thin), thin)
        return lax.dot_general(x, wg[:, rows], last, preferred_element_type=F32)

    whole = pl.ds(0, block)
    columns_of = [(wq, whole, WQ), (wk, whole, WK)] + [(wv, v_cols(p), WV + p) for p in range(halves)]
    early = 3
    landed(gains, load_sem.at[GAINS])
    x_own, squares = chunk(tp)
    pending = None
    for n, (w, cols, sem) in enumerate(columns_of[:early]):
        landed(w.at[:, cols], load_sem.at[sem])
        made = product(x_own, tp, w, cols)
        if pending is not None:
            own_part[n - 1] = pending
        pending = made
    landed(wg, load_sem.at[WG])
    gates_own = gate_part(x_own, tp)
    own_part[early - 1] = pending
    gsnd[:, 0, : 2 * gate_count] = gates_own
    landed(tokall.at[pl.ds(0, n_tp - 1)], tok_r.at[0])
    others = [((tp + t) % n_tp, chunk((tp + t) % n_tp)) for t in range(1, n_tp)]
    for _, (_, more) in others:
        squares = squares + more

    def rs_copy(to, p):
        return pltpu.make_async_remote_copy(
            src_ref=snd.at[to, p], dst_ref=rcv.at[kv, p],
            send_sem=sent_sem.at[RS_S], recv_sem=rs_r.at[min(p, 2)],
            device_id=(dp, to, tp), device_id_type=MESH)

    def gate_copy(to):
        return pltpu.make_async_remote_copy(
            src_ref=gsnd.at[to], dst_ref=grcv.at[kv],
            send_sem=sent_sem.at[GATE_S], recv_sem=rs_r.at[3],
            device_id=(dp, to, tp), device_id_type=MESH)

    def send_part(p, total):
        for h in range(heads):
            part[:, p * heads + h, :] = total[:, h * LANES : (h + 1) * LANES]
        for to in range(n_kv):
            snd[to, p] = part[to, p * heads : (p + 1) * heads, :].astype(BF16)
        for to in far_first:
            rs_copy(to, p).start()

    def mate_sum(of):
        total = None
        for t, (x_t, _) in others:
            made = of(x_t, t)
            total = made if total is None else total + made
        return total

    def mate_part(p):
        w, cols, _ = columns_of[p]
        return mate_sum(lambda x_t, t: product(x_t, t, w, cols))

    pending = mate_part(0)
    for p in range(1, len(columns_of)):
        w, cols, sem = columns_of[p]
        if p < early:
            made = mate_part(p)
        else:
            landed(w.at[:, cols], load_sem.at[sem])
            made = product(x_own, tp, w, cols)
        if p == early - 1:
            gates_mate = mate_sum(gate_part)
        send_part(p - 1, pending + own_part[p - 1])
        if p == early - 1:
            gsnd[:, 0, : 2 * gate_count] = gsnd[:, 0, : 2 * gate_count] + gates_mate
            gsnd[:, 1, :] = jnp.broadcast_to(squares, (n_kv, LANES))
            for to in far_first:
                gate_copy(to).start()
        pending = made if p < early else made + mate_part(p)
    send_part(len(columns_of) - 1, pending)

    landed(bias, load_sem.at[BIAS])
    landed(nrm, load_sem.at[NRM])
    landed(stb, load_sem.at[STB])
    landed(mem, load_sem.at[MEM])
    membf[...] = mem[...].astype(BF16).reshape(heads * dv, dqk)

    lane = lax.broadcasted_iota(jnp.int32, (heads, LANES), 1)
    sub = lax.broadcasted_iota(jnp.int32, (heads, LANES), 0)
    own_head = sub + tp * heads

    def column(row, at):
        wide = jnp.pad(row, ((0, 0), (0, LANES - row.shape[1]))) if row.shape[1] < LANES else row
        picked = jnp.where(lane == own_head + at, jnp.broadcast_to(wide, lane.shape), 0.0)
        return jnp.sum(picked, axis=1, keepdims=True)

    peers = [(kv + o) % n_kv for o in range(1, n_kv)]

    def joined(p):
        total = part[kv, p * heads : (p + 1) * heads, :]
        for o in peers:
            total = total + rcv[o, p].astype(F32)
        return total

    landed(grcv.at[pl.ds(0, n_kv - 1)], rs_r.at[3])
    gate_sum = gsnd[kv]
    for o in peers:
        gate_sum = gate_sum + grcv[o]
    scale = lax.rsqrt(gate_sum[1:2] * (1.0 / width) + norm_eps)
    gate_row = gate_sum[0:1] * scale
    gate_i = column(gate_row, 0) + column(bias[0], 0)
    gate_f = column(gate_row, gate_count) + column(bias[1], 0)
    landed(rcv.at[pl.ds(0, n_kv - 1), 0], rs_r.at[0])
    q = joined(0) * scale * dqk**-0.5
    log_forget = jnp.minimum(gate_f, 0.0) - jnp.log1p(jnp.exp(-jnp.abs(gate_f)))
    stab_wide = jnp.broadcast_to(stb[...], (heads, heads))
    eye = (lax.broadcasted_iota(jnp.int32, (heads, heads), 0)
           == lax.broadcasted_iota(jnp.int32, (heads, heads), 1))
    stab = jnp.sum(jnp.where(eye, stab_wide, 0.0), axis=1, keepdims=True)
    carried = log_forget + stab
    new_stab = jnp.maximum(carried, gate_i)
    keep = jnp.exp(carried - new_stab)
    fresh = jnp.exp(gate_i - new_stab)
    ostb[...] = jnp.sum(jnp.where(eye, jnp.broadcast_to(new_stab, (heads, heads)), 0.0), axis=0, keepdims=True)
    norm_dot = jnp.sum(nrm[...] * q, axis=1, keepdims=True)
    q_hi = q.astype(BF16)
    q_lo = (q - q_hi.astype(F32)).astype(BF16)
    wide_recall = lax.dot_general(
        jnp.concatenate([q_hi, q_lo], axis=0), membf[...], (((1,), (1,)), ((), ())),
        preferred_element_type=F32)
    wide_recall = wide_recall[:heads] + wide_recall[heads:]
    row_id = lax.broadcasted_iota(jnp.int32, (heads, dv), 0)
    recall = jnp.zeros((heads, dv), F32)
    for h in range(heads):
        recall = jnp.where(row_id == h, wide_recall[:, h * dv : (h + 1) * dv], recall)
    landed(rcv.at[pl.ds(0, n_kv - 1), 1], rs_r.at[1])
    k = joined(1) * scale
    match = jnp.sum(q * k, axis=1, keepdims=True)
    denominator = keep * norm_dot + fresh * match
    floor_value = jnp.maximum(jnp.abs(denominator), jnp.exp(-new_stab))
    landed(rcv.at[pl.ds(0, n_kv - 1), pl.ds(2, halves)], rs_r.at[2])
    for p in range(halves):
        vrow[p * heads : (p + 1) * heads, :] = joined(2 + p) * scale
    v = jnp.concatenate([vrow[pl.ds(s, heads, stride=halves), :] for s in range(halves)], axis=1)
    cell = (keep * recall + (fresh * match) * v) / floor_value
    cell = cell.astype(BF16)
    cell_own[...] = cell

    for to in far_first:
        pltpu.make_async_remote_copy(
            src_ref=cell_own, dst_ref=cell_all.at[kv], send_sem=sent_sem.at[CELL_S], recv_sem=cell_r.at[0],
            device_id=(dp, to, tp), device_id_type=MESH).start()
    cell_all[kv] = cell
    onrm[0] = keep * nrm[...] + fresh * k
    fresh_v = fresh * v
    fresh_vt = fresh_v.T
    for h in range(heads):
        newmem[0, h] = keep[h : h + 1] * mem[h] + fresh_vt[:, h : h + 1] * k[h : h + 1]
    landed(wo, load_sem.at[WO])
    landed(wup, load_sem.at[WUP])
    landed(tokall.at[pl.ds(0, n_all - n_tp)], tok_r.at[1])
    landed(cell_all.at[pl.ds(0, n_kv - 1)], cell_r.at[0])
    cells = cell_all[...].astype(F32)
    rows = jnp.concatenate([cells[:, h, :] for h in range(heads)], axis=1).astype(BF16)

    def lagged(jobs):
        pending = None
        for make, finish in jobs:
            made = make()
            if pending is not None:
                pending[1](pending[0])
            pending = made, finish
        pending[1](pending[0])

    def send_y(c):
        def finish(total):
            y = total.astype(BF16)
            y_own[c] = y
            for to in far_first + [kv]:
                for t in range(n_tp):
                    if t or to is not kv:
                        to_tp = (tp + t) % n_tp
                        pltpu.make_async_remote_copy(
                            src_ref=y_own.at[c], dst_ref=y_all.at[g, c],
                            send_sem=sent_sem.at[Y_S], recv_sem=y_r.at[kv, c],
                            device_id=(dp, to, to_tp), device_id_type=MESH).start()
            y_all[g, c] = y

        return finish

    def y_job(c):
        cols = slice(c * thin, (c + 1) * thin)
        return lambda: jnp.dot(rows, wo[:, cols], preferred_element_type=F32), send_y(c)

    lagged([y_job(c) for c in range(n_tp)])

    square_sum = jnp.zeros((batch, 1), F32)
    total_up = [None, None]
    cut = hidden // 2
    for i, j in enumerate(chips):
        if i == n_kv - 1:
            landed(wdn, load_sem.at[WDN])
        for wanted in ([list(range(n_tp))] if i < n_kv - 1 else [[c] for c in range(n_tp)]):
            mixed = []
            for c in wanted:
                count = n_tp if i > 0 else n_tp - 1
                landed(y_all.at[pl.ds(0, count), c], y_r.at[j, c])
                base = tokall[j * n_tp + c].astype(F32)
                for t in range(n_tp):
                    base = base + y_all[j * n_tp + t, c].astype(F32)
                m = base.astype(BF16).astype(F32)
                if i == 0:
                    mid[c] = m
                cols = pl.ds(pl.multiple_of((j * n_tp + c) * thin, thin), thin)
                mixed.append((m * gains[1, :, cols]).astype(BF16))
                square_sum = square_sum + jnp.sum(m * m, axis=1, keepdims=True)
            at = pl.multiple_of((j * n_tp + wanted[0]) * thin, thin)
            wide = jnp.concatenate(mixed, axis=1) if len(mixed) > 1 else mixed[0]
            for s in range(2):
                more = jnp.dot(
                    wide, wup[pl.ds(at, len(wanted) * thin), s * cut : (s + 1) * cut],
                    preferred_element_type=F32)
                total_up[s] = more if total_up[s] is None else total_up[s] + more
    scale2 = lax.rsqrt(square_sum * (1.0 / width) + norm_eps)

    def activated(total):
        up = jnp.maximum(total * scale2, 0.0)
        return (up * up).astype(BF16)

    targets = [chips[i] * n_tp + (tp + t) % n_tp for i in reversed(range(n_kv)) for t in reversed(range(n_tp))]

    def send_down(to):
        def finish(total):
            stage[to] = total.astype(BF16)
            pltpu.make_async_remote_copy(
                src_ref=stage.at[to], dst_ref=land.at[g],
                send_sem=sent_sem.at[DN_S], recv_sem=dn_r.at[0],
                device_id=(dp, to // n_tp, to % n_tp), device_id_type=MESH).start()

        return finish

    own_down = []
    act_low, act_high = activated(total_up[0]), activated(total_up[1])

    def down_job(n, to):
        def make():
            cols = pl.ds(pl.multiple_of(to * thin, thin), thin)
            low = jnp.dot(act_low, wdn[:cut, cols], preferred_element_type=F32)
            return low + jnp.dot(act_high, wdn[cut:, cols], preferred_element_type=F32)

        return make, send_down(to) if n < len(targets) - 1 else own_down.append

    lagged([down_job(n, to) for n, to in enumerate(targets)])
    total = own_down[0] + mid[tp]

    landed(tokall.at[pl.ds(0, n_all - 1)], sent_sem.at[TOK_S])
    landed(snd.at[pl.ds(0, n_kv - 1)], sent_sem.at[RS_S])
    landed(gsnd.at[pl.ds(0, n_kv - 1)], sent_sem.at[GATE_S])
    landed(cell_all.at[pl.ds(0, n_kv - 1)], sent_sem.at[CELL_S])
    landed(y_all.at[pl.ds(0, n_all - 1)], sent_sem.at[Y_S])
    landed(land.at[pl.ds(0, n_all - 1)], dn_r.at[0])
    for o in range(1, n_all):
        total = total + land[(g + o) % n_all].astype(F32)
    otok[...] = total.astype(BF16)
    landed(stage.at[pl.ds(0, n_all - 1)], sent_sem.at[DN_S])


def hand_over(a, b, c, d, out_a, out_b, out_c, out_d, sems):
    pairs = ((b, out_b), (a, out_a), (c, out_c), (d, out_d))
    copies = [pltpu.make_async_copy(x, y, sems.at[i]) for i, (x, y) in enumerate(pairs)]
    for c in copies:
        c.start()
    for c in copies:
        c.wait()


def fits_fused(tokens, w_query, w_value, memory, w_output, w_up, w_down, n_kv, n_tp):
    own_rows, heads, dv, dqk = memory.shape
    batch, thin = tokens.shape
    span = w_query.shape[0]
    held = 2 * (2 * w_query.size + w_value.size + w_output.size + w_up.size + w_down.size)
    held += 10 * memory.size
    return (
        own_rows == 1 and batch == n_kv and heads == 8 and dqk == LANES and dv % LANES == 0
        and w_query.shape[1] == heads * dqk and w_value.shape[1] == heads * dv
        and thin % (2 * LANES) == 0 and span == n_tp * thin and n_kv >= 2 and n_tp >= 2
        and w_output.shape[1] == span and held < 52 * 2**20
    )


def fused_on_device(
    tokens, mix_gain, w_query, w_key, w_value, w_igate, w_fgate, igate_bias, fgate_bias,
    memory, normalizer, stabilizer, w_output, mlp_gain, w_up, w_down,
):
    n_kv = lax.axis_size("kv")
    n_tp = lax.axis_size("tp")
    n_all = n_kv * n_tp
    batch, thin = tokens.shape
    _, heads, dv, dqk = memory.shape
    span = w_query.shape[0]
    width = n_all * thin
    halves = dv // LANES
    hbm_spec = pl.BlockSpec(memory_space=pltpu.HBM)
    vmem_spec = pl.BlockSpec(memory_space=pltpu.VMEM)
    vm = pltpu.VMEM
    dma = pltpu.SemaphoreType.DMA
    scratch = [
        vm((batch, thin), BF16),
        vm((n_all, batch, thin), BF16),
        vm((2, 1, width), F32),
        vm(w_query.shape, BF16),
        vm(w_key.shape, BF16),
        vm(w_value.shape, BF16),
        vm((2 * w_igate.shape[1], span), BF16),
        vm((2, 1, igate_bias.shape[0]), F32),
        vm((heads, dv, dqk), F32),
        vm((heads * dv, dqk), BF16),
        vm((heads, dqk), F32),
        vm((1, heads), F32),
        vm(w_output.shape, BF16),
        vm(w_up.shape, BF16),
        vm(w_down.shape, BF16),
        vm((3, batch, heads * LANES), F32),
        vm((n_kv, (2 + halves) * heads, LANES), F32),
        vm((n_kv, 2 + halves, heads, LANES), BF16),
        vm((n_kv, 2 + halves, heads, LANES), BF16),
        vm((n_kv, 2, LANES), F32),
        vm((n_kv, 2, LANES), F32),
        vm((halves * heads, LANES), F32),
        vm((heads, dv), BF16),
        vm((n_kv, heads, dv), BF16),
        vm((n_tp, batch, thin), BF16),
        vm((n_all, n_tp, batch, thin), BF16),
        vm((n_tp, batch, thin), F32),
        vm((n_all, batch, thin), BF16),
        vm((n_all, batch, thin), BF16),
        dma((12 + halves,)), dma((6,)),
        dma((2,)), dma((4,)), dma((1,)), dma((n_kv, n_tp)), dma((1,)),
    ]
    args = (
        tokens, mix_gain.reshape(1, -1), w_query, w_key, w_value, w_igate.T, w_fgate.T,
        igate_bias.reshape(1, -1), fgate_bias.reshape(1, -1), memory, normalizer, stabilizer,
        w_output, mlp_gain.reshape(1, -1), w_up, w_down,
    )
    args = [pltpu.with_memory_space_constraint(a, pltpu.HBM) for a in args]
    results = pl.pallas_call(
        functools.partial(fused_cell, n_kv, n_tp),
        out_shape=(
            jax.ShapeDtypeStruct(tokens.shape, BF16),
            jax.ShapeDtypeStruct(memory.shape, F32),
            jax.ShapeDtypeStruct(normalizer.shape, F32),
            jax.ShapeDtypeStruct(stabilizer.shape, F32),
        ),
        in_specs=[hbm_spec] * 16,
        out_specs=(vmem_spec,) * 4,
        scratch_shapes=scratch,
        compiler_params=pltpu.CompilerParams(
            collective_id=0, has_side_effects=True, vmem_limit_bytes=52 * 2**20
        ),
        name="fused_cell",
    )(*args)
    return pl.pallas_call(
        hand_over,
        out_shape=tuple(jax.ShapeDtypeStruct(r.shape, r.dtype) for r in results),
        in_specs=[vmem_spec] * 4,
        out_specs=(hbm_spec,) * 4,
        scratch_shapes=[dma((4,))],
        compiler_params=pltpu.CompilerParams(vmem_limit_bytes=2**20),
        name="hand_over",
    )(*results)


def routed(*arrays):
    tokens, w_query, w_value, memory = arrays[0], arrays[2], arrays[4], arrays[9]
    w_output, w_up, w_down = arrays[12], arrays[14], arrays[15]
    n_kv, n_tp = lax.axis_size("kv"), lax.axis_size("tp")
    if fits_fused(tokens, w_query, w_value, memory, w_output, w_up, w_down, n_kv, n_tp):
        return fused_on_device(*arrays)
    return on_device(*arrays)


def solution(mesh):
    in_specs = (
        P("dp", ("kv", "tp")),
        P(),
        P("kv", "tp"),
        P("kv", "tp"),
        P("kv", "tp"),
        P(),
        P(),
        P(),
        P(),
        P(("dp", "kv"), "tp", None, None),
        P(("dp", "kv"), "tp", None),
        P(("dp", "kv"), "tp"),
        P("tp", "kv"),
        P(),
        P(None, ("kv", "tp")),
        P(("kv", "tp"), None),
    )
    out_specs = (
        P("dp", ("kv", "tp")),
        P(("dp", "kv"), "tp", None, None),
        P(("dp", "kv"), "tp", None),
        P(("dp", "kv"), "tp"),
    )
    return jax.shard_map(
        routed, mesh=mesh, in_specs=in_specs, out_specs=out_specs, check_vma=False
    )
```

```python
import functools

import jax
import jax.numpy as jnp
from jax import lax
from jax.experimental import pallas as pl
from jax.experimental.pallas import tpu as pltpu
from jax.sharding import PartitionSpec as P

MESH = pl.DeviceIdType.MESH
F32 = jnp.float32
BF16 = jnp.bfloat16
LANES = 128


norm_eps = 1e-06


def rms_normed(rows, gain):
    wide_rows = rows.astype(jnp.float32)
    scale = lax.rsqrt(jnp.mean(wide_rows * wide_rows, axis=-1, keepdims=True) + norm_eps)
    return (wide_rows * scale * gain).astype(jnp.bfloat16)


def on_device(
    tokens,
    mix_gain,
    w_query,
    w_key,
    w_value,
    w_igate,
    w_fgate,
    igate_bias,
    fgate_bias,
    memory,
    normalizer,
    stabilizer,
    w_output,
    mlp_gain,
    w_up,
    w_down,
):
    DV, DQK = memory.shape[2:]
    kv_count = lax.axis_size("kv")
    tp_count = lax.axis_size("tp")
    kv_index = lax.axis_index("kv")
    tp_index = lax.axis_index("tp")
    own_rows = memory.shape[0]
    head_count = memory.shape[1]
    whole_rows = lax.all_gather(tokens, ("kv", "tp"), axis=1, tiled=True)
    batch_rows = whole_rows.shape[0]
    wide_rows = whole_rows.astype(jnp.float32)
    normed = rms_normed(whole_rows, mix_gain)
    row_span = w_query.shape[0]
    own_cols = lax.dynamic_slice_in_dim(normed, kv_index * row_span, row_span, 1)
    joined = lax.psum_scatter(
        jnp.concatenate(
            [
                jnp.dot(own_cols, w_query, preferred_element_type=jnp.float32),
                jnp.dot(own_cols, w_key, preferred_element_type=jnp.float32),
                jnp.dot(own_cols, w_value, preferred_element_type=jnp.float32),
            ],
            axis=1,
        ),
        "kv",
        scatter_dimension=0,
        tiled=True,
    )
    query_cols = w_query.shape[1]
    queries = joined[:, :query_cols].reshape(own_rows, head_count, DQK) * DQK ** (-0.5)
    key_rows = joined[:, query_cols : 2 * query_cols].reshape(own_rows, head_count, DQK)
    values = joined[:, 2 * query_cols :].reshape(own_rows, head_count, DV)
    own_normed = lax.dynamic_slice_in_dim(normed, kv_index * own_rows, own_rows, 0)
    igate_cols = lax.dynamic_slice_in_dim(w_igate, tp_index * head_count, head_count, 1)
    fgate_cols = lax.dynamic_slice_in_dim(w_fgate, tp_index * head_count, head_count, 1)
    ibias_own = lax.dynamic_slice_in_dim(igate_bias, tp_index * head_count, head_count, 0)
    fbias_own = lax.dynamic_slice_in_dim(fgate_bias, tp_index * head_count, head_count, 0)
    input_gate = jnp.dot(own_normed, igate_cols, preferred_element_type=jnp.float32) + ibias_own
    log_forget = jax.nn.log_sigmoid(
        jnp.dot(own_normed, fgate_cols, preferred_element_type=jnp.float32) + fbias_own
    )
    carried = log_forget + stabilizer
    new_stabilizer = jnp.maximum(carried, input_gate)
    keep_weight = jnp.exp(carried - new_stabilizer)
    fresh_weight = jnp.exp(input_gate - new_stabilizer)
    recall = jnp.einsum("bhvd,bhd->bhv", memory, queries, precision=lax.Precision.HIGHEST)
    match_score = jnp.sum(queries * key_rows, axis=-1)
    numerator = keep_weight[..., None] * recall + (fresh_weight * match_score)[..., None] * values
    denominator = keep_weight * jnp.sum(normalizer * queries, axis=-1) + fresh_weight * match_score
    floor_value = jnp.maximum(jnp.abs(denominator), jnp.exp(-new_stabilizer))
    cell_out = (
        (numerator / floor_value[..., None]).astype(jnp.bfloat16).reshape(own_rows, head_count * DV)
    )
    new_memory = (
        keep_weight[..., None, None] * memory
        + fresh_weight[..., None, None] * values[..., :, None] * key_rows[..., None, :]
    )
    new_normalizer = keep_weight[..., None] * normalizer + fresh_weight[..., None] * key_rows
    partial_value = jnp.dot(
        lax.all_gather(cell_out, "kv", axis=0, tiled=True),
        w_output,
        preferred_element_type=jnp.float32,
    )
    block_cols = partial_value.shape[1]
    pieces = lax.all_gather(
        partial_value.astype(jnp.bfloat16)[:, None, :], ("kv", "tp"), axis=1, tiled=True
    )
    summed = jnp.sum(
        pieces.astype(jnp.float32).reshape(batch_rows, kv_count, tp_count, block_cols), axis=2
    )
    middle = (wide_rows + summed.reshape(batch_rows, kv_count * block_cols)).astype(jnp.bfloat16)
    mixer_in = rms_normed(middle, mlp_gain)
    up_rows = jnp.dot(mixer_in, w_up, preferred_element_type=jnp.float32)
    activation = jnp.square(jax.nn.relu(up_rows)).astype(jnp.bfloat16)
    thin_cols = tokens.shape[1]
    down_cols = lax.psum_scatter(
        lax.dot_general(
            w_down, activation, (((0,), (1,)), ((), ())), preferred_element_type=jnp.float32
        ),
        ("kv", "tp"),
        scatter_dimension=0,
        tiled=True,
    )
    middle_own = lax.dynamic_slice_in_dim(
        middle, (kv_index * tp_count + tp_index) * thin_cols, thin_cols, 1
    )
    new_tokens = (middle_own.astype(jnp.float32) + down_cols.T).astype(jnp.bfloat16)
    return (new_tokens, new_memory, new_normalizer, new_stabilizer)


def landed(ref, sem):
    pltpu.make_async_copy(ref, ref, sem).wait()


def fused_cell(
    n_kv,
    n_tp,
    tok_h, mixg_h, wq_h, wk_h, wv_h, wig_h, wfg_h, ib_h, fb_h,
    mem_h, nrm_h, stb_h, wo_h, mlpg_h, wup_h, wdn_h,
    otok, newmem, onrm, ostb,
    tok, tokall, gains, wq, wk, wv, wg, bias,
    mem, membf, nrm, stb, wo, wup, wdn,
    own_part, part, rcv, gsnd, grcv, v_own, v_snd, v_all, v_rows, v_head, cell_own, cell_all, y_own, y_all, mid, stage, land,
    load_sem, sent_sem, tok_r, rs_r, cell_r, y_r, dn_r,
):
    dp = lax.axis_index("dp")
    kv = lax.axis_index("kv")
    tp = lax.axis_index("tp")
    n_all = n_kv * n_tp
    g = kv * n_tp + tp
    batch, thin = tok.shape
    span = wq.shape[0]
    heads, dv, dqk = mem.shape
    width = n_all * thin
    halves = dv // LANES
    gate_count = wg.shape[0] // 2
    block = heads * LANES
    hidden = wup.shape[1]

    own_span = pl.ds(pl.multiple_of(kv * span, span), span)

    def v_cols(p):
        return pl.ds(p * block, block)

    far_side = kv // 2
    near = kv + far_side * (3 - 2 * kv)

    def chip(i):
        if n_kv == 4:
            step = (i + near) % 3 if i < 3 else i
            return 3 * far_side + (1 - 2 * far_side) * step
        return (kv + i) % n_kv

    chips = [kv] + [chip(i) for i in range(1, n_kv)]
    far_first = chips[:0:-1]

    def up_rows(j):
        return pl.ds(pl.multiple_of(j * span, span), span)

    TOK, GAINS, WQ, WK, WG, BIAS, NRM, STB, MEM, WO, WUP, WDN, WV = range(13)
    loads = [
        (tok_h, tok, TOK), (mixg_h, gains.at[0], GAINS), (mlpg_h, gains.at[1], GAINS), (wq_h, wq, WQ),
        (wk_h, wk, WK),
        (wig_h.at[:, own_span], wg.at[pl.ds(0, gate_count)], WG),
        (wfg_h.at[:, own_span], wg.at[pl.ds(gate_count, gate_count)], WG),
    ]
    loads += [(wv_h.at[:, v_cols(p)], wv.at[:, v_cols(p)], WV + p) for p in range(halves)]
    loads += [
        (ib_h, bias.at[0], BIAS), (fb_h, bias.at[1], BIAS), (nrm_h.at[0], nrm, NRM), (stb_h, stb, STB),
        (mem_h.at[0], mem, MEM), (wo_h, wo, WO),
    ]
    loads += [(wup_h.at[up_rows(j)], wup.at[up_rows(j)], WUP) for j in chips]
    loads += [(wdn_h, wdn, WDN)]
    load = [pltpu.make_async_copy(x, y, load_sem.at[n]) for x, y, n in loads]

    for c in load[:4]:
        c.start()
    barrier = pltpu.get_barrier_semaphore()
    for to in far_first:
        for t in range(n_tp):
            pl.semaphore_signal(barrier, inc=1, device_id=(dp, to, t), device_id_type=MESH)
    for t in range(1, n_tp):
        pl.semaphore_signal(barrier, inc=1, device_id=(dp, kv, (tp + t) % n_tp), device_id_type=MESH)
    for c in load[4:]:
        c.start()

    gsnd[...] = jnp.zeros(gsnd.shape, F32)
    landed(tok, load_sem.at[TOK])
    pl.semaphore_wait(barrier, n_all - 1)

    def tok_copy(to, to_tp, n):
        return pltpu.make_async_remote_copy(
            src_ref=tok, dst_ref=tokall.at[g], send_sem=sent_sem.at[0], recv_sem=tok_r.at[n],
            device_id=(dp, to, to_tp), device_id_type=MESH)

    for t in range(1, n_tp):
        tok_copy(kv, (tp + t) % n_tp, 0).start()
    tokall[g] = tok[...]
    for to in far_first:
        for t in range(n_tp):
            tok_copy(to, (tp + t) % n_tp, 1).start()

    def chunk(t):
        cols = pl.ds(pl.multiple_of((kv * n_tp + t) * thin, thin), thin)
        raw = tokall[kv * n_tp + t].astype(F32)
        scaled = raw * gains[0, :, cols]
        high = scaled.astype(BF16).astype(F32)
        both = jnp.concatenate([high, scaled - high], axis=0).astype(BF16)
        return both, jnp.sum(raw * raw, axis=1, keepdims=True)

    def folded(total):
        return total[:batch] + total[batch:]

    def product(x, t, w):
        rows = pl.ds(pl.multiple_of(t * thin, thin), thin)
        return jnp.dot(x, w[rows, :], preferred_element_type=F32)

    landed(gains, load_sem.at[GAINS])
    x_own, _ = chunk(tp)
    landed(wq, load_sem.at[WQ])
    own_part[0] = product(x_own, tp, wq)
    landed(wk, load_sem.at[WK])
    own_part[1] = product(x_own, tp, wk)
    landed(wg, load_sem.at[WG])
    landed(tokall.at[pl.ds(0, n_tp - 1)], tok_r.at[0])
    chunks = [chunk(t) for t in range(n_tp)]
    x = jnp.concatenate([c for c, _ in chunks], axis=1)
    squares = chunks[0][1]
    for _, more in chunks[1:]:
        squares = squares + more

    def mate_part(w):
        total = None
        for t in range(1, n_tp):
            made = product(chunk((tp + t) % n_tp)[0], (tp + t) % n_tp, w)
            total = made if total is None else total + made
        return total

    def rs_copy(to, p):
        return pltpu.make_async_remote_copy(
            src_ref=part.at[to, pl.ds(p * heads, heads)], dst_ref=rcv.at[kv, pl.ds(p * heads, heads)],
            send_sem=sent_sem.at[0], recv_sem=rs_r.at[p],
            device_id=(dp, to, tp), device_id_type=MESH)

    def gate_copy(to):
        return pltpu.make_async_remote_copy(
            src_ref=gsnd.at[to], dst_ref=grcv.at[kv],
            send_sem=sent_sem.at[0], recv_sem=rs_r.at[3],
            device_id=(dp, to, tp), device_id_type=MESH)

    def send_part(p, total):
        for h in range(heads):
            part[:, p * heads + h, :] = total[:, h * LANES : (h + 1) * LANES]
        for to in far_first:
            rs_copy(to, p).start()

    gates = lax.dot_general(x, wg[...], (((1,), (1,)), ((), ())), preferred_element_type=F32)
    q_mate = mate_part(wq)
    k_mate = mate_part(wk)
    gsnd[:, 0, : 2 * gate_count] = folded(gates)
    gsnd[:, 1, :] = jnp.broadcast_to(squares, (n_kv, LANES))
    for to in far_first:
        gate_copy(to).start()
    send_part(0, folded(q_mate + own_part[0]))
    send_part(1, folded(k_mate + own_part[1]))
    for p in range(halves):
        landed(wv.at[:, v_cols(p)], load_sem.at[WV + p])
        made = folded(jnp.dot(x, wv[:, v_cols(p)], preferred_element_type=F32))
        v_own[p] = made
        v_snd[p] = made.astype(BF16)
        for to in far_first:
            pltpu.make_async_remote_copy(
                src_ref=v_snd.at[p], dst_ref=v_all.at[kv, p],
                send_sem=sent_sem.at[0], recv_sem=rs_r.at[2],
                device_id=(dp, to, tp), device_id_type=MESH).start()

    landed(bias, load_sem.at[BIAS])
    landed(nrm, load_sem.at[NRM])
    landed(stb, load_sem.at[STB])
    landed(mem, load_sem.at[MEM])
    membf[...] = mem[...].astype(BF16).reshape(heads * dv, dqk)

    lane = lax.broadcasted_iota(jnp.int32, (heads, LANES), 1)
    sub = lax.broadcasted_iota(jnp.int32, (heads, LANES), 0)
    own_head = sub + tp * heads

    def column(row, at):
        wide = jnp.pad(row, ((0, 0), (0, LANES - row.shape[1]))) if row.shape[1] < LANES else row
        picked = jnp.where(lane == own_head + at, jnp.broadcast_to(wide, lane.shape), 0.0)
        return jnp.sum(picked, axis=1, keepdims=True)

    peers = [(kv + o) % n_kv for o in range(1, n_kv)]

    def joined(p):
        total = part[kv, p * heads : (p + 1) * heads, :]
        for o in peers:
            total = total + rcv[o, p * heads : (p + 1) * heads, :]
        return total

    landed(grcv.at[pl.ds(0, n_kv - 1)], rs_r.at[3])
    gate_sum = gsnd[kv]
    for o in peers:
        gate_sum = gate_sum + grcv[o]
    scale = lax.rsqrt(gate_sum[1:2] * (1.0 / width) + norm_eps)
    gate_row = gate_sum[0:1] * scale
    gate_i = column(gate_row, 0) + column(bias[0], 0)
    gate_f = column(gate_row, gate_count) + column(bias[1], 0)
    landed(rcv.at[pl.ds(0, n_kv - 1), pl.ds(0, heads)], rs_r.at[0])
    q = joined(0) * scale * dqk**-0.5
    log_forget = jnp.minimum(gate_f, 0.0) - jnp.log1p(jnp.exp(-jnp.abs(gate_f)))
    stab_wide = jnp.broadcast_to(stb[...], (heads, heads))
    eye = (lax.broadcasted_iota(jnp.int32, (heads, heads), 0)
           == lax.broadcasted_iota(jnp.int32, (heads, heads), 1))
    stab = jnp.sum(jnp.where(eye, stab_wide, 0.0), axis=1, keepdims=True)
    carried = log_forget + stab
    new_stab = jnp.maximum(carried, gate_i)
    keep = jnp.exp(carried - new_stab)
    fresh = jnp.exp(gate_i - new_stab)
    ostb[...] = jnp.sum(jnp.where(eye, jnp.broadcast_to(new_stab, (heads, heads)), 0.0), axis=0, keepdims=True)
    norm_dot = jnp.sum(nrm[...] * q, axis=1, keepdims=True)
    q_hi = q.astype(BF16)
    q_lo = (q - q_hi.astype(F32)).astype(BF16)
    wide_recall = lax.dot_general(
        jnp.concatenate([q_hi, q_lo], axis=0), membf[...], (((1,), (1,)), ((), ())),
        preferred_element_type=F32)
    wide_recall = wide_recall[:heads] + wide_recall[heads:]
    row_id = lax.broadcasted_iota(jnp.int32, (heads, dv), 0)
    recall = jnp.zeros((heads, dv), F32)
    for h in range(heads):
        recall = jnp.where(row_id == h, wide_recall[:, h * dv : (h + 1) * dv], recall)
    landed(rcv.at[pl.ds(0, n_kv - 1), pl.ds(heads, heads)], rs_r.at[1])
    k = joined(1) * scale
    match = jnp.sum(q * k, axis=1, keepdims=True)
    denominator = keep * norm_dot + fresh * match
    floor_value = jnp.maximum(jnp.abs(denominator), jnp.exp(-new_stab))
    cell_own[:, :dv] = keep * recall / floor_value
    cell_own[:, dv:] = (fresh * match / floor_value) * scale
    for to in far_first:
        pltpu.make_async_remote_copy(
            src_ref=cell_own, dst_ref=cell_all.at[kv], send_sem=sent_sem.at[0], recv_sem=cell_r.at[0],
            device_id=(dp, to, tp), device_id_type=MESH).start()
    cell_all[kv] = cell_own[...]
    onrm[0] = keep * nrm[...] + fresh * k
    landed(v_all.at[pl.ds(0, n_kv - 1)], rs_r.at[2])
    for p in range(halves):
        v_sum = v_own[p]
        for o in peers:
            v_sum = v_sum + v_all[o, p].astype(F32)
        v_rows[:, v_cols(p)] = v_sum
    own_row = v_rows[pl.ds(kv, 1), :]
    for h in range(heads):
        v_head[h : h + 1, :] = own_row[:, h * dv : (h + 1) * dv]
    fresh_v = (fresh * scale[:, :1]) * v_head[...]
    fresh_vt = fresh_v.T
    for h in range(heads):
        newmem[0, h] = keep[h : h + 1] * mem[h] + fresh_vt[:, h : h + 1] * k[h : h + 1]
    landed(wo, load_sem.at[WO])
    landed(wup, load_sem.at[WUP])
    landed(tokall.at[pl.ds(0, n_all - n_tp)], tok_r.at[1])
    landed(cell_all.at[pl.ds(0, n_kv - 1)], cell_r.at[0])
    rows = []
    for h in range(heads):
        weight = cell_all[:, h, dv:]
        for s in range(halves):
            at = h * dv + s * LANES
            row = cell_all[:, h, s * LANES : (s + 1) * LANES] + weight * v_rows[:, at : at + LANES]
            rows.append(row.astype(BF16))
    rows = jnp.concatenate(rows, axis=1)

    def lagged(jobs):
        pending = None
        for make, finish in jobs:
            made = make()
            if pending is not None:
                pending[1](pending[0])
            pending = made, finish
        pending[1](pending[0])

    def y_copy(c, to, t):
        span_of = slice(None) if c is None else c
        return pltpu.make_async_remote_copy(
            src_ref=y_own.at[span_of], dst_ref=y_all.at[g, span_of],
            send_sem=sent_sem.at[0], recv_sem=y_r.at[kv],
            device_id=(dp, to, t), device_id_type=MESH)

    def send_y(c):
        def finish(total):
            y = total.astype(BF16)
            y_own[c] = y
            for t in range(n_tp):
                y_copy(c, chips[1], t).start()
            for t in range(1, n_tp):
                y_copy(c, kv, (tp + t) % n_tp).start()
            y_all[g, c] = y

        return finish

    def y_job(c):
        cols = slice(c * thin, (c + 1) * thin)
        return lambda: jnp.dot(rows, wo[:, cols], preferred_element_type=F32), send_y(c)

    lagged([y_job(c) for c in range(n_tp)])
    for to in chips[2:]:
        for t in range(n_tp):
            y_copy(None, to, t).start()

    square_sum = jnp.zeros((batch, 1), F32)
    total_up = [None, None]
    cut = hidden // 2
    for i, j in enumerate(chips):
        if i == n_kv - 1:
            landed(wdn, load_sem.at[WDN])
        landed(y_all.at[pl.ds(0, n_tp if i > 0 else n_tp - 1)], y_r.at[j])
        for wanted in ([list(range(n_tp))] if i < n_kv - 1 else [[c] for c in range(n_tp)]):
            mixed = []
            for c in wanted:
                base = tokall[j * n_tp + c].astype(F32)
                for t in range(n_tp):
                    base = base + y_all[j * n_tp + t, c].astype(F32)
                m = base.astype(BF16).astype(F32)
                if i == 0:
                    mid[c] = m
                cols = pl.ds(pl.multiple_of((j * n_tp + c) * thin, thin), thin)
                mixed.append((m * gains[1, :, cols]).astype(BF16))
                square_sum = square_sum + jnp.sum(m * m, axis=1, keepdims=True)
            at = pl.multiple_of((j * n_tp + wanted[0]) * thin, thin)
            wide = jnp.concatenate(mixed, axis=1) if len(mixed) > 1 else mixed[0]
            for s in range(2):
                more = jnp.dot(
                    wide, wup[pl.ds(at, len(wanted) * thin), s * cut : (s + 1) * cut],
                    preferred_element_type=F32)
                total_up[s] = more if total_up[s] is None else total_up[s] + more
    scale2 = lax.rsqrt(square_sum * (1.0 / width) + norm_eps)

    def activated(total):
        up = jnp.maximum(total * scale2, 0.0)
        return (up * up).astype(BF16)

    targets = [to * n_tp + t for to in far_first for t in range(n_tp)]
    targets += [kv * n_tp + (tp + t) % n_tp for t in reversed(range(n_tp))]

    def send_down(to):
        def finish(total):
            stage[to] = total.astype(BF16)
            pltpu.make_async_remote_copy(
                src_ref=stage.at[to], dst_ref=land.at[g],
                send_sem=sent_sem.at[0], recv_sem=dn_r.at[0],
                device_id=(dp, to // n_tp, to % n_tp), device_id_type=MESH).start()

        return finish

    own_down = []
    act_low, act_high = activated(total_up[0]), activated(total_up[1])

    def down_job(n, to):
        def make():
            cols = pl.ds(pl.multiple_of(to * thin, thin), thin)
            low = jnp.dot(act_low, wdn[:cut, cols], preferred_element_type=F32)
            return low + jnp.dot(act_high, wdn[cut:, cols], preferred_element_type=F32)

        return make, send_down(to) if n < len(targets) - 1 else own_down.append

    down_jobs = [down_job(n, to) for n, to in enumerate(targets)]
    down_jobs[0][1](down_jobs[0][0]())
    lagged(down_jobs[1:])
    total = own_down[0] + mid[tp]

    landed(land.at[pl.ds(0, n_all - 1)], dn_r.at[0])
    for o in range(1, n_all):
        total = total + land[(g + o) % n_all].astype(F32)
    otok[...] = total.astype(BF16)
    wide = (n_all - 1) * batch * (thin + span + thin) + (n_kv - 1) * halves * batch * block
    narrow = (n_kv - 1) * (2 * LANES + 2 * block + heads * (dv + LANES))
    sent = (wide + 2 * narrow) // dqk
    landed(membf.at[pl.ds(0, sent)], sent_sem.at[0])


def hand_over(a, b, c, d, out_a, out_b, out_c, out_d, sems):
    pairs = ((b, out_b), (a, out_a), (c, out_c), (d, out_d))
    copies = [pltpu.make_async_copy(x, y, sems.at[i]) for i, (x, y) in enumerate(pairs)]
    for c in copies:
        c.start()
    for c in copies:
        c.wait()


def fits_fused(tokens, w_query, w_value, memory, w_output, w_up, w_down, n_kv, n_tp):
    own_rows, heads, dv, dqk = memory.shape
    batch, thin = tokens.shape
    span = w_query.shape[0]
    held = 2 * (2 * w_query.size + w_value.size + w_output.size + w_up.size + w_down.size)
    held += 10 * memory.size
    return (
        own_rows == 1 and batch == n_kv and heads == 8 and dqk == LANES and dv % LANES == 0
        and w_query.shape[1] == heads * dqk and w_value.shape[1] == heads * dv
        and thin % (2 * LANES) == 0 and span == n_tp * thin and n_kv >= 2 and n_tp >= 2
        and w_output.shape[1] == span and held < 52 * 2**20
    )


def fused_on_device(
    tokens, mix_gain, w_query, w_key, w_value, w_igate, w_fgate, igate_bias, fgate_bias,
    memory, normalizer, stabilizer, w_output, mlp_gain, w_up, w_down,
):
    n_kv = lax.axis_size("kv")
    n_tp = lax.axis_size("tp")
    n_all = n_kv * n_tp
    batch, thin = tokens.shape
    _, heads, dv, dqk = memory.shape
    span = w_query.shape[0]
    width = n_all * thin
    halves = dv // LANES
    hbm_spec = pl.BlockSpec(memory_space=pltpu.HBM)
    vmem_spec = pl.BlockSpec(memory_space=pltpu.VMEM)
    vm = pltpu.VMEM
    dma = pltpu.SemaphoreType.DMA
    scratch = [
        vm((batch, thin), BF16),
        vm((n_all, batch, thin), BF16),
        vm((2, 1, width), F32),
        vm(w_query.shape, BF16),
        vm(w_key.shape, BF16),
        vm(w_value.shape, BF16),
        vm((2 * w_igate.shape[1], span), BF16),
        vm((2, 1, igate_bias.shape[0]), F32),
        vm((heads, dv, dqk), F32),
        vm((heads * dv, dqk), BF16),
        vm((heads, dqk), F32),
        vm((1, heads), F32),
        vm(w_output.shape, BF16),
        vm(w_up.shape, BF16),
        vm(w_down.shape, BF16),
        vm((2, 2 * batch, heads * LANES), F32),
        vm((n_kv, 2 * heads, LANES), F32),
        vm((n_kv, 2 * heads, LANES), F32),
        vm((n_kv, 2, LANES), F32),
        vm((n_kv, 2, LANES), F32),
        vm((halves, batch, heads * LANES), F32),
        vm((halves, batch, heads * LANES), BF16),
        vm((n_kv, halves, batch, heads * LANES), BF16),
        vm((batch, heads * dv), F32),
        vm((heads, dv), F32),
        vm((heads, dv + LANES), F32),
        vm((n_kv, heads, dv + LANES), F32),
        vm((n_tp, batch, thin), BF16),
        vm((n_all, n_tp, batch, thin), BF16),
        vm((n_tp, batch, thin), F32),
        vm((n_all, batch, thin), BF16),
        vm((n_all, batch, thin), BF16),
        dma((12 + halves,)), dma((1,)),
        dma((2,)), dma((4,)), dma((1,)), dma((n_kv,)), dma((1,)),
    ]
    args = (
        tokens, mix_gain.reshape(1, -1), w_query, w_key, w_value, w_igate.T, w_fgate.T,
        igate_bias.reshape(1, -1), fgate_bias.reshape(1, -1), memory, normalizer, stabilizer,
        w_output, mlp_gain.reshape(1, -1), w_up, w_down,
    )
    args = [pltpu.with_memory_space_constraint(a, pltpu.HBM) for a in args]
    results = pl.pallas_call(
        functools.partial(fused_cell, n_kv, n_tp),
        out_shape=(
            jax.ShapeDtypeStruct(tokens.shape, BF16),
            jax.ShapeDtypeStruct(memory.shape, F32),
            jax.ShapeDtypeStruct(normalizer.shape, F32),
            jax.ShapeDtypeStruct(stabilizer.shape, F32),
        ),
        in_specs=[hbm_spec] * 16,
        out_specs=(vmem_spec,) * 4,
        scratch_shapes=scratch,
        compiler_params=pltpu.CompilerParams(
            collective_id=0, has_side_effects=True, vmem_limit_bytes=52 * 2**20
        ),
        name="fused_cell",
    )(*args)
    return pl.pallas_call(
        hand_over,
        out_shape=tuple(jax.ShapeDtypeStruct(r.shape, r.dtype) for r in results),
        in_specs=[vmem_spec] * 4,
        out_specs=(hbm_spec,) * 4,
        scratch_shapes=[dma((4,))],
        compiler_params=pltpu.CompilerParams(vmem_limit_bytes=2**20),
        name="hand_over",
    )(*results)


def routed(*arrays):
    tokens, w_query, w_value, memory = arrays[0], arrays[2], arrays[4], arrays[9]
    w_output, w_up, w_down = arrays[12], arrays[14], arrays[15]
    n_kv, n_tp = lax.axis_size("kv"), lax.axis_size("tp")
    if fits_fused(tokens, w_query, w_value, memory, w_output, w_up, w_down, n_kv, n_tp):
        return fused_on_device(*arrays)
    return on_device(*arrays)


def solution(mesh):
    in_specs = (
        P("dp", ("kv", "tp")),
        P(),
        P("kv", "tp"),
        P("kv", "tp"),
        P("kv", "tp"),
        P(),
        P(),
        P(),
        P(),
        P(("dp", "kv"), "tp", None, None),
        P(("dp", "kv"), "tp", None),
        P(("dp", "kv"), "tp"),
        P("tp", "kv"),
        P(),
        P(None, ("kv", "tp")),
        P(("kv", "tp"), None),
    )
    out_specs = (
        P("dp", ("kv", "tp")),
        P(("dp", "kv"), "tp", None, None),
        P(("dp", "kv"), "tp", None),
        P(("dp", "kv"), "tp"),
    )
    return jax.shard_map(
        routed, mesh=mesh, in_specs=in_specs, out_specs=out_specs, check_vma=False
    )
```

```python
import functools

import jax
import jax.numpy as jnp
from jax import lax
from jax.experimental import pallas as pl
from jax.experimental.pallas import tpu as pltpu
from jax.sharding import PartitionSpec as P

MESH = pl.DeviceIdType.MESH
F32 = jnp.float32
BF16 = jnp.bfloat16
LANES = 128


norm_eps = 1e-06


def rms_normed(rows, gain):
    wide_rows = rows.astype(jnp.float32)
    scale = lax.rsqrt(jnp.mean(wide_rows * wide_rows, axis=-1, keepdims=True) + norm_eps)
    return (wide_rows * scale * gain).astype(jnp.bfloat16)


def on_device(
    tokens,
    mix_gain,
    w_query,
    w_key,
    w_value,
    w_igate,
    w_fgate,
    igate_bias,
    fgate_bias,
    memory,
    normalizer,
    stabilizer,
    w_output,
    mlp_gain,
    w_up,
    w_down,
):
    DV, DQK = memory.shape[2:]
    kv_count = lax.axis_size("kv")
    tp_count = lax.axis_size("tp")
    kv_index = lax.axis_index("kv")
    tp_index = lax.axis_index("tp")
    own_rows = memory.shape[0]
    head_count = memory.shape[1]
    whole_rows = lax.all_gather(tokens, ("kv", "tp"), axis=1, tiled=True)
    batch_rows = whole_rows.shape[0]
    wide_rows = whole_rows.astype(jnp.float32)
    normed = rms_normed(whole_rows, mix_gain)
    row_span = w_query.shape[0]
    own_cols = lax.dynamic_slice_in_dim(normed, kv_index * row_span, row_span, 1)
    joined = lax.psum_scatter(
        jnp.concatenate(
            [
                jnp.dot(own_cols, w_query, preferred_element_type=jnp.float32),
                jnp.dot(own_cols, w_key, preferred_element_type=jnp.float32),
                jnp.dot(own_cols, w_value, preferred_element_type=jnp.float32),
            ],
            axis=1,
        ),
        "kv",
        scatter_dimension=0,
        tiled=True,
    )
    query_cols = w_query.shape[1]
    queries = joined[:, :query_cols].reshape(own_rows, head_count, DQK) * DQK ** (-0.5)
    key_rows = joined[:, query_cols : 2 * query_cols].reshape(own_rows, head_count, DQK)
    values = joined[:, 2 * query_cols :].reshape(own_rows, head_count, DV)
    own_normed = lax.dynamic_slice_in_dim(normed, kv_index * own_rows, own_rows, 0)
    igate_cols = lax.dynamic_slice_in_dim(w_igate, tp_index * head_count, head_count, 1)
    fgate_cols = lax.dynamic_slice_in_dim(w_fgate, tp_index * head_count, head_count, 1)
    ibias_own = lax.dynamic_slice_in_dim(igate_bias, tp_index * head_count, head_count, 0)
    fbias_own = lax.dynamic_slice_in_dim(fgate_bias, tp_index * head_count, head_count, 0)
    input_gate = jnp.dot(own_normed, igate_cols, preferred_element_type=jnp.float32) + ibias_own
    log_forget = jax.nn.log_sigmoid(
        jnp.dot(own_normed, fgate_cols, preferred_element_type=jnp.float32) + fbias_own
    )
    carried = log_forget + stabilizer
    new_stabilizer = jnp.maximum(carried, input_gate)
    keep_weight = jnp.exp(carried - new_stabilizer)
    fresh_weight = jnp.exp(input_gate - new_stabilizer)
    recall = jnp.einsum("bhvd,bhd->bhv", memory, queries, precision=lax.Precision.HIGHEST)
    match_score = jnp.sum(queries * key_rows, axis=-1)
    numerator = keep_weight[..., None] * recall + (fresh_weight * match_score)[..., None] * values
    denominator = keep_weight * jnp.sum(normalizer * queries, axis=-1) + fresh_weight * match_score
    floor_value = jnp.maximum(jnp.abs(denominator), jnp.exp(-new_stabilizer))
    cell_out = (
        (numerator / floor_value[..., None]).astype(jnp.bfloat16).reshape(own_rows, head_count * DV)
    )
    new_memory = (
        keep_weight[..., None, None] * memory
        + fresh_weight[..., None, None] * values[..., :, None] * key_rows[..., None, :]
    )
    new_normalizer = keep_weight[..., None] * normalizer + fresh_weight[..., None] * key_rows
    partial_value = jnp.dot(
        lax.all_gather(cell_out, "kv", axis=0, tiled=True),
        w_output,
        preferred_element_type=jnp.float32,
    )
    block_cols = partial_value.shape[1]
    pieces = lax.all_gather(
        partial_value.astype(jnp.bfloat16)[:, None, :], ("kv", "tp"), axis=1, tiled=True
    )
    summed = jnp.sum(
        pieces.astype(jnp.float32).reshape(batch_rows, kv_count, tp_count, block_cols), axis=2
    )
    middle = (wide_rows + summed.reshape(batch_rows, kv_count * block_cols)).astype(jnp.bfloat16)
    mixer_in = rms_normed(middle, mlp_gain)
    up_rows = jnp.dot(mixer_in, w_up, preferred_element_type=jnp.float32)
    activation = jnp.square(jax.nn.relu(up_rows)).astype(jnp.bfloat16)
    thin_cols = tokens.shape[1]
    down_cols = lax.psum_scatter(
        lax.dot_general(
            w_down, activation, (((0,), (1,)), ((), ())), preferred_element_type=jnp.float32
        ),
        ("kv", "tp"),
        scatter_dimension=0,
        tiled=True,
    )
    middle_own = lax.dynamic_slice_in_dim(
        middle, (kv_index * tp_count + tp_index) * thin_cols, thin_cols, 1
    )
    new_tokens = (middle_own.astype(jnp.float32) + down_cols.T).astype(jnp.bfloat16)
    return (new_tokens, new_memory, new_normalizer, new_stabilizer)


def landed(ref, sem):
    pltpu.make_async_copy(ref, ref, sem).wait()


def fused_cell(
    n_kv,
    n_tp,
    tok_h, mixg_h, wq_h, wk_h, wv_h, wig_h, wfg_h, ib_h, fb_h,
    mem_h, nrm_h, stb_h, wo_h, mlpg_h, wup_h, wdn_h,
    otok, newmem, onrm, ostb,
    tok, tokall, gains, wq, wk, wv, wg, bias,
    mem, membf, nrm, stb, wo, wup, wdn,
    part, rcv, gsnd, grcv, v_own, v_snd, v_all, v_rows, v_head, cell_own, cell_all, y_own, y_all, mid, stage, land,
    load_sem, sent_sem, tok_r, rs_r, cell_r, y_r, dn_r, pair_sem,
):
    dp = lax.axis_index("dp")
    kv = lax.axis_index("kv")
    tp = lax.axis_index("tp")
    n_all = n_kv * n_tp
    g = kv * n_tp + tp
    batch, thin = tok.shape
    span = wq.shape[0]
    heads, dv, dqk = mem.shape
    width = n_all * thin
    halves = dv // LANES
    gate_count = wg.shape[0] // 2
    block = heads * LANES
    hidden = wup.shape[1]

    own_span = pl.ds(pl.multiple_of(kv * span, span), span)

    def v_cols(p):
        return pl.ds(p * block, block)

    far_side = kv // 2
    near = kv + far_side * (3 - 2 * kv)

    def chip(i):
        if n_kv == 4:
            step = (i + near) % 3 if i < 3 else i
            return 3 * far_side + (1 - 2 * far_side) * step
        return (kv + i) % n_kv

    chips = [kv] + [chip(i) for i in range(1, n_kv)]
    far_first = chips[:0:-1]
    down_first, y_first = far_first, chips[1:]
    if n_kv == 4:
        low = near * (1 - far_side)
        swap = low * (far_first[1] - far_first[0])
        down_first = [far_first[0] + swap, far_first[1] - swap, far_first[2]]
        y_first = [near * a + (1 - near) * b for a, b in zip(chips[1:], far_first)]

    def up_rows(j):
        return pl.ds(pl.multiple_of(j * span, span), span)

    TOK, GAINS, WQ, WK, WG, BIAS, NRM, STB, MEM, WO, WUP, WDN, WDN_REST, WV = range(14)
    loads = [
        (tok_h, tok, TOK), (mixg_h, gains.at[0], GAINS), (mlpg_h, gains.at[1], GAINS), (wq_h, wq, WQ),
        (wig_h.at[:, own_span], wg.at[pl.ds(0, gate_count)], WG),
        (wfg_h.at[:, own_span], wg.at[pl.ds(gate_count, gate_count)], WG),
        (wk_h, wk, WK),
    ]
    loads += [(wv_h.at[:, v_cols(p)], wv.at[:, v_cols(p)], WV + p) for p in range(halves)]
    loads += [
        (ib_h, bias.at[0], BIAS), (fb_h, bias.at[1], BIAS), (nrm_h.at[0], nrm, NRM), (stb_h, stb, STB),
        (mem_h.at[0], mem, MEM), (wo_h, wo, WO),
    ]
    loads += [(wup_h.at[up_rows(j)], wup.at[up_rows(j)], WUP) for j in chips]
    for n, to in enumerate(down_first + [kv]):
        loads += [(wdn_h.at[:, up_rows(to)], wdn.at[:, up_rows(to)], WDN_REST if n else WDN)]
    load = [pltpu.make_async_copy(x, y, load_sem.at[n]) for x, y, n in loads]

    barrier = pltpu.get_barrier_semaphore()
    mate = (dp, kv, 1 - tp)

    def signal(sem, to):
        pl.semaphore_signal(sem, inc=1, device_id=to, device_id_type=MESH)

    @pl.when(tp == 0)
    def _():
        signal(barrier, mate)

    for c in load:
        c.start()

    @pl.when(tp == 1)
    def _():
        pl.semaphore_wait(barrier, 1)
        signal(pair_sem, mate)

    @pl.when(tp == 0)
    def _():
        pl.semaphore_wait(pair_sem, 1)
        for to in far_first:
            signal(barrier, (dp, to, 0))

    gsnd[...] = jnp.zeros(gsnd.shape, F32)
    landed(tok, load_sem.at[TOK])

    def tok_copy(to, to_tp, n):
        return pltpu.make_async_remote_copy(
            src_ref=tok, dst_ref=tokall.at[g], send_sem=sent_sem.at[0], recv_sem=tok_r.at[n],
            device_id=(dp, to, to_tp), device_id_type=MESH)

    for t in range(1, n_tp):
        tok_copy(kv, (tp + t) % n_tp, 0).start()
    tokall[g] = tok[...]

    def chunk(t):
        cols = pl.ds(pl.multiple_of((kv * n_tp + t) * thin, thin), thin)
        raw = tokall[kv * n_tp + t].astype(F32)
        scaled = raw * gains[0, :, cols]
        high = scaled.astype(BF16).astype(F32)
        both = jnp.concatenate([high, scaled - high], axis=0).astype(BF16)
        return both, jnp.sum(raw * raw, axis=1, keepdims=True)

    def folded(total):
        return total[:batch] + total[batch:]

    landed(gains, load_sem.at[GAINS])
    landed(tokall.at[pl.ds(0, n_tp - 1)], tok_r.at[0])
    chunks = [chunk(t) for t in range(n_tp)]
    x = jnp.concatenate([c for c, _ in chunks], axis=1)
    squares = chunks[0][1]
    for _, more in chunks[1:]:
        squares = squares + more

    def rs_copy(to, p):
        return pltpu.make_async_remote_copy(
            src_ref=part.at[to, pl.ds(p * heads, heads)], dst_ref=rcv.at[kv, pl.ds(p * heads, heads)],
            send_sem=sent_sem.at[0], recv_sem=rs_r.at[p],
            device_id=(dp, to, tp), device_id_type=MESH)

    def gate_copy(to):
        return pltpu.make_async_remote_copy(
            src_ref=gsnd.at[to], dst_ref=grcv.at[kv],
            send_sem=sent_sem.at[0], recv_sem=rs_r.at[3],
            device_id=(dp, to, tp), device_id_type=MESH)

    def keep_part(p, total):
        for h in range(heads):
            part[:, p * heads + h, :] = total[:, h * LANES : (h + 1) * LANES]

    def first_sends():
        @pl.when(tp == 0)
        def _():
            pl.semaphore_wait(barrier, n_kv - 1)
            signal(pair_sem, mate)

        @pl.when(tp == 1)
        def _():
            pl.semaphore_wait(pair_sem, 1)

        for to in far_first:
            gate_copy(to).start()
        for to in far_first:
            rs_copy(to, 0).start()

    landed(wq, load_sem.at[WQ])
    q_all = jnp.dot(x, wq[...], preferred_element_type=F32)
    landed(wg, load_sem.at[WG])
    gates = lax.dot_general(x, wg[...], (((1,), (1,)), ((), ())), preferred_element_type=F32)
    gsnd[:, 0, : 2 * gate_count] = folded(gates)
    gsnd[:, 1, :] = jnp.broadcast_to(squares, (n_kv, LANES))
    keep_part(0, folded(q_all))

    @pl.when(2 * kv >= n_kv)
    def _():
        first_sends()

    landed(wk, load_sem.at[WK])
    keep_part(1, folded(jnp.dot(x, wk[...], preferred_element_type=F32)))

    @pl.when(2 * kv < n_kv)
    def _():
        first_sends()

    for to in far_first:
        rs_copy(to, 1).start()
    for to in far_first:
        for t in range(n_tp):
            tok_copy(to, (tp + t) % n_tp, 1).start()
    for p in range(halves):
        landed(wv.at[:, v_cols(p)], load_sem.at[WV + p])
        made = folded(jnp.dot(x, wv[:, v_cols(p)], preferred_element_type=F32))
        v_own[p] = made
        v_snd[p] = made.astype(BF16)
        for to in far_first:
            pltpu.make_async_remote_copy(
                src_ref=v_snd.at[p], dst_ref=v_all.at[kv, p],
                send_sem=sent_sem.at[0], recv_sem=rs_r.at[2],
                device_id=(dp, to, tp), device_id_type=MESH).start()

    landed(bias, load_sem.at[BIAS])
    landed(nrm, load_sem.at[NRM])
    landed(stb, load_sem.at[STB])
    landed(mem, load_sem.at[MEM])
    membf[...] = mem[...].astype(BF16).reshape(heads * dv, dqk)

    lane = lax.broadcasted_iota(jnp.int32, (heads, LANES), 1)
    sub = lax.broadcasted_iota(jnp.int32, (heads, LANES), 0)
    own_head = sub + tp * heads

    def column(row, at):
        wide = jnp.pad(row, ((0, 0), (0, LANES - row.shape[1]))) if row.shape[1] < LANES else row
        picked = jnp.where(lane == own_head + at, jnp.broadcast_to(wide, lane.shape), 0.0)
        return jnp.sum(picked, axis=1, keepdims=True)

    peers = [(kv + o) % n_kv for o in range(1, n_kv)]

    def joined(p):
        total = part[kv, p * heads : (p + 1) * heads, :]
        for o in peers:
            total = total + rcv[o, p * heads : (p + 1) * heads, :]
        return total

    landed(grcv.at[pl.ds(0, n_kv - 1)], rs_r.at[3])
    gate_sum = gsnd[kv]
    for o in peers:
        gate_sum = gate_sum + grcv[o]
    scale = lax.rsqrt(gate_sum[1:2] * (1.0 / width) + norm_eps)
    gate_row = gate_sum[0:1] * scale
    gate_i = column(gate_row, 0) + column(bias[0], 0)
    gate_f = column(gate_row, gate_count) + column(bias[1], 0)
    landed(rcv.at[pl.ds(0, n_kv - 1), pl.ds(0, heads)], rs_r.at[0])
    q = joined(0) * scale * dqk**-0.5
    log_forget = jnp.minimum(gate_f, 0.0) - jnp.log1p(jnp.exp(-jnp.abs(gate_f)))
    stab_wide = jnp.broadcast_to(stb[...], (heads, heads))
    eye = (lax.broadcasted_iota(jnp.int32, (heads, heads), 0)
           == lax.broadcasted_iota(jnp.int32, (heads, heads), 1))
    stab = jnp.sum(jnp.where(eye, stab_wide, 0.0), axis=1, keepdims=True)
    carried = log_forget + stab
    new_stab = jnp.maximum(carried, gate_i)
    keep = jnp.exp(carried - new_stab)
    fresh = jnp.exp(gate_i - new_stab)
    ostb[...] = jnp.sum(jnp.where(eye, jnp.broadcast_to(new_stab, (heads, heads)), 0.0), axis=0, keepdims=True)
    norm_dot = jnp.sum(nrm[...] * q, axis=1, keepdims=True)
    q_hi = q.astype(BF16)
    q_lo = (q - q_hi.astype(F32)).astype(BF16)
    wide_recall = lax.dot_general(
        jnp.concatenate([q_hi, q_lo], axis=0), membf[...], (((1,), (1,)), ((), ())),
        preferred_element_type=F32)
    wide_recall = wide_recall[:heads] + wide_recall[heads:]
    row_id = lax.broadcasted_iota(jnp.int32, (heads, dv), 0)
    recall = jnp.zeros((heads, dv), F32)
    for h in range(heads):
        recall = jnp.where(row_id == h, wide_recall[:, h * dv : (h + 1) * dv], recall)
    landed(rcv.at[pl.ds(0, n_kv - 1), pl.ds(heads, heads)], rs_r.at[1])
    k = joined(1) * scale
    match = jnp.sum(q * k, axis=1, keepdims=True)
    denominator = keep * norm_dot + fresh * match
    floor_value = jnp.maximum(jnp.abs(denominator), jnp.exp(-new_stab))
    cell_own[:, :dv] = keep * recall / floor_value
    cell_own[:, dv:] = (fresh * match / floor_value) * scale
    for to in far_first:
        pltpu.make_async_remote_copy(
            src_ref=cell_own, dst_ref=cell_all.at[kv], send_sem=sent_sem.at[0], recv_sem=cell_r.at[0],
            device_id=(dp, to, tp), device_id_type=MESH).start()
    cell_all[kv] = cell_own[...]
    onrm[0] = keep * nrm[...] + fresh * k
    landed(v_all.at[pl.ds(0, n_kv - 1)], rs_r.at[2])
    for p in range(halves):
        v_sum = v_own[p]
        for o in peers:
            v_sum = v_sum + v_all[o, p].astype(F32)
        v_rows[:, v_cols(p)] = v_sum
    own_row = v_rows[pl.ds(kv, 1), :]
    for h in range(heads):
        v_head[h : h + 1, :] = own_row[:, h * dv : (h + 1) * dv]
    fresh_v = (fresh * scale[:, :1]) * v_head[...]
    fresh_vt = fresh_v.T
    for h in range(heads):
        newmem[0, h] = keep[h : h + 1] * mem[h] + fresh_vt[:, h : h + 1] * k[h : h + 1]
    landed(wo, load_sem.at[WO])
    landed(tokall.at[pl.ds(0, n_all - n_tp)], tok_r.at[1])
    landed(cell_all.at[pl.ds(0, n_kv - 1)], cell_r.at[0])
    rows = []
    for h in range(heads):
        weight = cell_all[:, h, dv:]
        for s in range(halves):
            at = h * dv + s * LANES
            row = cell_all[:, h, s * LANES : (s + 1) * LANES] + weight * v_rows[:, at : at + LANES]
            rows.append(row.astype(BF16))
    rows = jnp.concatenate(rows, axis=1)

    def lagged(jobs):
        pending = None
        for make, finish in jobs:
            made = make()
            if pending is not None:
                pending[1](pending[0])
            pending = made, finish
        pending[1](pending[0])

    def send_y(c):
        def finish(total):
            y = total.astype(BF16)
            y_own[c] = y
            for to in y_first[:1] + [kv] + y_first[1:]:
                for t in range(1 if to is kv else 0, n_tp):
                    pltpu.make_async_remote_copy(
                        src_ref=y_own.at[c], dst_ref=y_all.at[g, c],
                        send_sem=sent_sem.at[0], recv_sem=y_r.at[kv, c],
                        device_id=(dp, to, (tp + t) % n_tp if to is kv else t), device_id_type=MESH).start()
            y_all[g, c] = y

        return finish

    def y_job(c):
        cols = slice(c * thin, (c + 1) * thin)
        return lambda: jnp.dot(rows, wo[:, cols], preferred_element_type=F32), send_y(c)

    lagged([y_job(c) for c in range(n_tp)])

    landed(wup, load_sem.at[WUP])
    square_sum = jnp.zeros((batch, 1), F32)
    total_up = [None, None]
    cut = hidden // 2
    for i, j in enumerate(chips):
        if i == n_kv - 1:
            landed(wdn.at[:, pl.ds(0, span)], load_sem.at[WDN])
        whole = i == 0 or 1 < i < n_kv - 1
        for wanted in ([list(range(n_tp))] if whole else [[c] for c in range(n_tp)]):
            for c in wanted:
                landed(y_all.at[pl.ds(0, n_tp if i > 0 else n_tp - 1), c], y_r.at[j, c])
            mixed = []
            for c in wanted:
                base = tokall[j * n_tp + c].astype(F32)
                for t in range(n_tp):
                    base = base + y_all[j * n_tp + t, c].astype(F32)
                m = base.astype(BF16).astype(F32)
                if i == 0:
                    mid[c] = m
                cols = pl.ds(pl.multiple_of((j * n_tp + c) * thin, thin), thin)
                mixed.append((m * gains[1, :, cols]).astype(BF16))
                square_sum = square_sum + jnp.sum(m * m, axis=1, keepdims=True)
            at = pl.multiple_of((j * n_tp + wanted[0]) * thin, thin)
            wide = jnp.concatenate(mixed, axis=1) if len(mixed) > 1 else mixed[0]
            for s in range(2):
                more = jnp.dot(
                    wide, wup[pl.ds(at, len(wanted) * thin), s * cut : (s + 1) * cut],
                    preferred_element_type=F32)
                total_up[s] = more if total_up[s] is None else total_up[s] + more
    scale2 = lax.rsqrt(square_sum * (1.0 / width) + norm_eps)

    def activated(total):
        up = jnp.maximum(total * scale2, 0.0)
        return (up * up).astype(BF16)

    targets = [to * n_tp + t for to in down_first for t in range(n_tp)]
    targets += [kv * n_tp + (tp + t) % n_tp for t in reversed(range(n_tp))]

    def send_down(to):
        def finish(total):
            stage[to] = total.astype(BF16)
            pltpu.make_async_remote_copy(
                src_ref=stage.at[to], dst_ref=land.at[g],
                send_sem=sent_sem.at[0], recv_sem=dn_r.at[0],
                device_id=(dp, to // n_tp, to % n_tp), device_id_type=MESH).start()

        return finish

    own_down = []
    act_low, act_high = activated(total_up[0]), activated(total_up[1])

    def down_job(n, to):
        def make():
            cols = pl.ds(pl.multiple_of(to * thin, thin), thin)
            low = jnp.dot(act_low, wdn[:cut, cols], preferred_element_type=F32)
            return low + jnp.dot(act_high, wdn[cut:, cols], preferred_element_type=F32)

        return make, send_down(to) if n < len(targets) - 1 else own_down.append

    down_jobs = [down_job(n, to) for n, to in enumerate(targets)]
    down_jobs[0][1](down_jobs[0][0]())
    landed(wdn.at[:, pl.ds(0, (n_kv - 1) * span)], load_sem.at[WDN_REST])
    lagged(down_jobs[1:])
    total = own_down[0] + mid[tp]

    landed(land.at[pl.ds(0, n_all - 1)], dn_r.at[0])
    for o in range(1, n_all):
        total = total + land[(g + o) % n_all].astype(F32)
    otok[...] = total.astype(BF16)
    wide = (n_all - 1) * batch * (thin + span + thin) + (n_kv - 1) * halves * batch * block
    narrow = (n_kv - 1) * (2 * LANES + 2 * block + heads * (dv + LANES))
    sent = (wide + 2 * narrow) // dqk
    landed(membf.at[pl.ds(0, sent)], sent_sem.at[0])


def hand_over(a, b, c, d, out_a, out_b, out_c, out_d, sems):
    pairs = ((b, out_b), (a, out_a), (c, out_c), (d, out_d))
    copies = [pltpu.make_async_copy(x, y, sems.at[i]) for i, (x, y) in enumerate(pairs)]
    for c in copies:
        c.start()
    for c in copies:
        c.wait()


def fits_fused(tokens, w_query, w_value, memory, w_output, w_up, w_down, n_kv, n_tp):
    own_rows, heads, dv, dqk = memory.shape
    batch, thin = tokens.shape
    span = w_query.shape[0]
    held = 2 * (2 * w_query.size + w_value.size + w_output.size + w_up.size + w_down.size)
    held += 10 * memory.size
    return (
        own_rows == 1 and batch == n_kv and heads == 8 and dqk == LANES and dv % LANES == 0
        and w_query.shape[1] == heads * dqk and w_value.shape[1] == heads * dv
        and thin % (2 * LANES) == 0 and span == n_tp * thin and n_kv >= 2 and n_tp == 2
        and w_output.shape[1] == span and held < 52 * 2**20
    )


def fused_on_device(
    tokens, mix_gain, w_query, w_key, w_value, w_igate, w_fgate, igate_bias, fgate_bias,
    memory, normalizer, stabilizer, w_output, mlp_gain, w_up, w_down,
):
    n_kv = lax.axis_size("kv")
    n_tp = lax.axis_size("tp")
    n_all = n_kv * n_tp
    batch, thin = tokens.shape
    _, heads, dv, dqk = memory.shape
    span = w_query.shape[0]
    width = n_all * thin
    halves = dv // LANES
    hbm_spec = pl.BlockSpec(memory_space=pltpu.HBM)
    vmem_spec = pl.BlockSpec(memory_space=pltpu.VMEM)
    vm = pltpu.VMEM
    dma = pltpu.SemaphoreType.DMA
    scratch = [
        vm((batch, thin), BF16),
        vm((n_all, batch, thin), BF16),
        vm((2, 1, width), F32),
        vm(w_query.shape, BF16),
        vm(w_key.shape, BF16),
        vm(w_value.shape, BF16),
        vm((2 * w_igate.shape[1], span), BF16),
        vm((2, 1, igate_bias.shape[0]), F32),
        vm((heads, dv, dqk), F32),
        vm((heads * dv, dqk), BF16),
        vm((heads, dqk), F32),
        vm((1, heads), F32),
        vm(w_output.shape, BF16),
        vm(w_up.shape, BF16),
        vm(w_down.shape, BF16),
        vm((n_kv, 2 * heads, LANES), F32),
        vm((n_kv, 2 * heads, LANES), F32),
        vm((n_kv, 2, LANES), F32),
        vm((n_kv, 2, LANES), F32),
        vm((halves, batch, heads * LANES), F32),
        vm((halves, batch, heads * LANES), BF16),
        vm((n_kv, halves, batch, heads * LANES), BF16),
        vm((batch, heads * dv), F32),
        vm((heads, dv), F32),
        vm((heads, dv + LANES), F32),
        vm((n_kv, heads, dv + LANES), F32),
        vm((n_tp, batch, thin), BF16),
        vm((n_all, n_tp, batch, thin), BF16),
        vm((n_tp, batch, thin), F32),
        vm((n_all, batch, thin), BF16),
        vm((n_all, batch, thin), BF16),
        dma((13 + halves,)), dma((1,)),
        dma((2,)), dma((4,)), dma((1,)), dma((n_kv, n_tp)), dma((1,)),
        pltpu.SemaphoreType.REGULAR,
    ]
    args = (
        tokens, mix_gain.reshape(1, -1), w_query, w_key, w_value, w_igate.T, w_fgate.T,
        igate_bias.reshape(1, -1), fgate_bias.reshape(1, -1), memory, normalizer, stabilizer,
        w_output, mlp_gain.reshape(1, -1), w_up, w_down,
    )
    args = [pltpu.with_memory_space_constraint(a, pltpu.HBM) for a in args]
    results = pl.pallas_call(
        functools.partial(fused_cell, n_kv, n_tp),
        out_shape=(
            jax.ShapeDtypeStruct(tokens.shape, BF16),
            jax.ShapeDtypeStruct(memory.shape, F32),
            jax.ShapeDtypeStruct(normalizer.shape, F32),
            jax.ShapeDtypeStruct(stabilizer.shape, F32),
        ),
        in_specs=[hbm_spec] * 16,
        out_specs=(vmem_spec,) * 4,
        scratch_shapes=scratch,
        compiler_params=pltpu.CompilerParams(
            collective_id=0, has_side_effects=True, vmem_limit_bytes=52 * 2**20
        ),
        name="fused_cell",
    )(*args)
    return pl.pallas_call(
        hand_over,
        out_shape=tuple(jax.ShapeDtypeStruct(r.shape, r.dtype) for r in results),
        in_specs=[vmem_spec] * 4,
        out_specs=(hbm_spec,) * 4,
        scratch_shapes=[dma((4,))],
        compiler_params=pltpu.CompilerParams(vmem_limit_bytes=2**20),
        name="hand_over",
    )(*results)


def routed(*arrays):
    tokens, w_query, w_value, memory = arrays[0], arrays[2], arrays[4], arrays[9]
    w_output, w_up, w_down = arrays[12], arrays[14], arrays[15]
    n_kv, n_tp = lax.axis_size("kv"), lax.axis_size("tp")
    if fits_fused(tokens, w_query, w_value, memory, w_output, w_up, w_down, n_kv, n_tp):
        return fused_on_device(*arrays)
    return on_device(*arrays)


def solution(mesh):
    in_specs = (
        P("dp", ("kv", "tp")),
        P(),
        P("kv", "tp"),
        P("kv", "tp"),
        P("kv", "tp"),
        P(),
        P(),
        P(),
        P(),
        P(("dp", "kv"), "tp", None, None),
        P(("dp", "kv"), "tp", None),
        P(("dp", "kv"), "tp"),
        P("tp", "kv"),
        P(),
        P(None, ("kv", "tp")),
        P(("kv", "tp"), None),
    )
    out_specs = (
        P("dp", ("kv", "tp")),
        P(("dp", "kv"), "tp", None, None),
        P(("dp", "kv"), "tp", None),
        P(("dp", "kv"), "tp"),
    )
    return jax.shard_map(
        routed, mesh=mesh, in_specs=in_specs, out_specs=out_specs, check_vma=False
    )
```
